32 devices in a mesh: ep: 16 (over z, x, core), tp: 2 (over y).
Axes of the slice: x: 2, y: 2, z: 4, core: 2. Of those that a mesh axis runs over, the one named last changes fastest.
Arguments:
- tokens: bfloat16 [2048, 2048], P('ep'), may hold values from -6 to 6
- cotangent: bfloat16 [2048, 2048], P('ep'), may hold values from -1.796875 to 1.796875
- group_weight: float32 [2048], P('ep'), may hold values from 0.2 to 1
- expert_weight: float32 [2048, 2], P('ep'), may hold values from 0.1 to 0.9
- group_choice: int32 [2048], P('ep'), may hold values from 0 to 3, as said below
- local_choice: int32 [2048, 2], P('ep'), may hold values from 0 to 3, as said below
- w_gate: bfloat16 [16, 2048, 512], P('ep', None, 'tp'), may hold values from -0.125 to 0.125
- w_up: bfloat16 [16, 2048, 512], P('ep', None, 'tp'), may hold values from -0.125 to 0.125
- w_down: bfloat16 [16, 512, 2048], P('ep', 'tp'), may hold values from -0.25 to 0.25
Outputs:
- token_grad: float32 [2048, 2048], P('ep', 'tp')
- group_weight_grad: float32 [2048], P('ep')
- expert_weight_grad: float32 [2048, 2], P('ep')
- w_gate_grad: float32 [16, 2048, 512], P('ep', None, 'tp')
- w_up_grad: float32 [16, 2048, 512], P('ep', None, 'tp')
- w_down_grad: float32 [16, 512, 2048], P('ep', 'tp')
The draws below stay inside these ranges and needn't reach their ends.
Inputs may be any that keep to these rules, and one draw needn't show every extreme that they name: Among the 128 tokens of each device (aligned blocks of tokens), no expert 4 * group_choice + local_choice is named by more than 24 slots, and some expert is named by exactly 24 slots of every device. `local_choice`: the 2 local choices of a token differ.
All inputs are finite; a program needn't handle non-finite values.
Results may differ from the reference program's by a relative error of at most 0.006.
Values may be sent and summed in bfloat16 or wider, within the bound.
A program may use at most 64 MiB of HBM per device.

```python
import math
import jax
import jax.numpy as jnp
from jax import lax

D = 2048
F = 512
EPG = 4
TOP_K = 2
TOK_DEV = 128
TOKENS = 2048
EXPERTS = 16
GROUPS = 4
CAP = 24
N_EP = 16


def route_tables(key):
    folded = jax.random.fold_in(key, 11)
    key_hot, key_perm, key_order, key_shift, key_step = jax.random.split(folded, 5)
    block_count = TOKENS // TOK_DEV
    busiest = EPG * CAP // TOP_K
    hot_group = jax.random.randint(key_hot, (), 0, GROUPS, dtype=jnp.int32)
    arrange = jax.vmap(lambda member_key: jax.random.permutation(member_key, TOK_DEV))(jax.random.split(key_perm, block_count)).astype(jnp.int32)
    others = jax.vmap(lambda member_key: jax.random.permutation(member_key, GROUPS - 1))(jax.random.split(key_order, block_count)).astype(jnp.int32)
    places = jnp.arange(TOK_DEV, dtype=jnp.int32)
    beyond = jnp.maximum(places - busiest, 0)
    column_ids = jnp.broadcast_to(beyond % (GROUPS - 1), (block_count, TOK_DEV))
    other_pick = jnp.take_along_axis(others, column_ids, axis=1)
    other_group = other_pick + (other_pick >= hot_group).astype(jnp.int32)
    group_at = jnp.where(places[None, :] < busiest, hot_group, other_group)
    rank_at = jnp.where(places < busiest, places, beyond // (GROUPS - 1))[None, :]
    shifts = jax.random.randint(key_shift, (block_count, GROUPS), 0, EPG, dtype=jnp.int32)
    strides = jax.random.randint(key_step, (block_count, GROUPS), 1, EPG, dtype=jnp.int32)
    first_local = (rank_at + jnp.take_along_axis(shifts, group_at, axis=1)) % EPG
    stride_at = jnp.take_along_axis(strides, group_at, axis=1)
    local_at = (first_local[..., None] + jnp.arange(TOP_K, dtype=jnp.int32) * stride_at[..., None]) % EPG
    inverse = jnp.argsort(arrange, axis=1, stable=True).astype(jnp.int32)
    group_table = jnp.take_along_axis(group_at, inverse, axis=1)
    local_table = jnp.take_along_axis(local_at, inverse[..., None], axis=1)
    return (group_table.reshape(TOKENS).astype(jnp.int32), local_table.reshape(TOKENS, TOP_K).astype(jnp.int32))


def draw_group_choice(key, part):
    return route_tables(key)[0]


def draw_local_choice(key, part):
    return route_tables(key)[1]


def level_of(own_key, extent, cuts, smallest, high):
    level = 1.0
    for dim, shards_of in cuts:
        draws = jax.random.uniform(jax.random.fold_in(jax.random.fold_in(own_key, 6), dim), (shards_of,), jnp.float32, smallest / len(cuts), high / len(cuts))
        level = level * jnp.repeat(jnp.exp(draws), extent[dim] // shards_of).reshape((-1,) + (1,) * (len(extent) - 1 - dim))
    return level


def noise(own_key, dims, scale, bound, cuts=(), kind=jnp.bfloat16):
    values = jax.random.normal(own_key, dims, jnp.float32) * scale
    if len(cuts) > 0:
        values = level_of(own_key, dims, cuts, -0.22, 0.18) * values
    return jnp.clip(values, min=-bound, max=bound).astype(kind)


def setup_inputs(seed: int = 0) -> dict:
    keys = jax.random.split(jax.random.key(seed), 10)
    return {
        "tokens": noise(keys[0], (TOKENS, D), 1.0, 6.0, ((0, 16),)),
        "cotangent": noise(keys[1], (TOKENS, D), 0.3, 1.796875, ((0, 16),)),
        "group_weight": jnp.clip(jnp.exp(math.log(1.0) - 1.609438 * jax.random.uniform(keys[2], (TOKENS,), jnp.float32) ** level_of(keys[2], (TOKENS,), ((0, 16),), -0.2, 0.2)), 0.2, 1.0),
        "expert_weight": jnp.clip(0.1 + 0.79999997 * jax.random.uniform(keys[3], (TOKENS, TOP_K), jnp.float32) ** level_of(keys[3], (TOKENS, TOP_K), ((0, 16),), -0.2, 0.2), 0.1, 0.9),
        "group_choice": draw_group_choice(jax.random.fold_in(keys[9], 71), 0),
        "local_choice": draw_local_choice(jax.random.fold_in(keys[9], 71), 0),
        "w_gate": noise(keys[6], (EXPERTS, D, F), D ** -0.5, 0.125, ((0, 16), (2, 2))),
        "w_up": noise(keys[7], (EXPERTS, D, F), D ** -0.5, 0.125, ((0, 16), (2, 2))),
        "w_down": noise(keys[8], (EXPERTS, F, D), F ** -0.5, 0.25, ((0, 16), (1, 2))),
    }


def expert_backward(arrived, cot_rows, gate_rows, first, second, third):
    pre_gate = jnp.dot(arrived, first, preferred_element_type=jnp.float32)
    pre_up = jnp.dot(arrived, second, preferred_element_type=jnp.float32)
    back_hidden = jnp.dot(cot_rows, third.T, preferred_element_type=jnp.float32)
    sigma = jax.nn.sigmoid(pre_gate)
    swish = pre_gate * sigma
    hidden = swish * pre_up
    gate_part = jnp.sum(hidden * back_hidden, axis=1)
    gate_float = gate_rows.astype(jnp.float32)[:, None]
    scaled = gate_float * back_hidden
    grad_gate_pre = (scaled * pre_up * sigma * (1.0 + pre_gate * (1.0 - sigma))).astype(jnp.bfloat16)
    grad_up_pre = (scaled * swish).astype(jnp.bfloat16)
    weighted = (gate_float * hidden).astype(jnp.bfloat16)
    first_grad = jnp.dot(arrived.T, grad_gate_pre, preferred_element_type=jnp.float32)
    second_grad = jnp.dot(arrived.T, grad_up_pre, preferred_element_type=jnp.float32)
    third_grad = jnp.dot(weighted.T, cot_rows, preferred_element_type=jnp.float32)
    total = jnp.dot(grad_gate_pre, first.T, preferred_element_type=jnp.float32)
    total = total + jnp.dot(grad_up_pre, second.T, preferred_element_type=jnp.float32)
    row_grad = total.astype(jnp.bfloat16)
    return first_grad, second_grad, third_grad, row_grad, gate_part


def reference(tokens, cotangent, group_weight, expert_weight, group_choice, local_choice, w_gate, w_up, w_down):
    slot_total = TOKENS * TOP_K
    expert_of = (group_choice[:, None] * EPG + local_choice).reshape(slot_total).astype(jnp.int32)
    member = (expert_of[:, None] == jnp.arange(EXPERTS, dtype=jnp.int32)[None, :]).astype(jnp.int32)
    running = jnp.cumsum(member, axis=0).astype(jnp.int32) - 1
    position = jnp.sum(running * member, axis=1).astype(jnp.int32)
    buffer_rows = N_EP * CAP
    slot_ids = jnp.arange(slot_total, dtype=jnp.int32)
    owner = jnp.full((EXPERTS, buffer_rows), slot_total, jnp.int32).at[expert_of, position].set(slot_ids)
    gate_value = (group_weight[:, None] * expert_weight).astype(jnp.bfloat16).reshape(slot_total)

    def per_expert(index):
        chosen = owner[index]
        live = chosen < slot_total
        safe = jnp.minimum(chosen, slot_total - 1)
        token_ids = (safe // TOP_K).astype(jnp.int32)
        zero = jnp.zeros((), jnp.bfloat16)
        arrived = jnp.where(live[:, None], tokens[token_ids], zero)
        cot_rows = jnp.where(live[:, None], cotangent[token_ids], zero)
        gate_rows = jnp.where(live, gate_value[safe], zero)
        return expert_backward(arrived, cot_rows, gate_rows, w_gate[index], w_up[index], w_down[index])

    first_grad, second_grad, third_grad, row_grad, gate_part = lax.map(per_expert, jnp.arange(EXPERTS, dtype=jnp.int32))
    slot_grad = row_grad[expert_of, position].astype(jnp.float32)
    token_grad = jnp.sum(slot_grad.reshape(TOKENS, TOP_K, D), axis=1)
    held = lax.optimization_barrier(gate_part[expert_of, position].astype(jnp.bfloat16))
    gate_grad = held.astype(jnp.float32).reshape(TOKENS, TOP_K)
    group_grad = jnp.sum(expert_weight * gate_grad, axis=1)
    expert_grad = group_weight[:, None] * gate_grad
    return (token_grad, group_grad, expert_grad, first_grad, second_grad, third_grad)
```

```python
import jax
import jax.numpy as jnp
from jax import lax
from jax.sharding import Mesh, PartitionSpec as P

EPG = 4
LANES = 128


def shards(
    tokens, cotangent, group_weight, expert_weight, group_choice, local_choice, w_gate, w_up, w_down
):
    token_count, feature_count = tokens.shape
    pick_count = expert_weight.shape[1]
    group_count = lax.axis_size("g")
    lane_count = lax.axis_size("tp")
    expert_count = group_count * EPG
    capacity = pick_count * (3 * token_count // (2 * expert_count))
    group_cap = -(-(EPG * capacity // pick_count) // 16) * 16
    row_count = group_count * group_cap
    piece = feature_count // lane_count
    order = jnp.arange(token_count, dtype=jnp.int32)
    same = (group_choice[:, None] == group_choice[None, :]) & (order[:, None] > order[None, :])
    dest = group_choice * group_cap + jnp.sum(same.astype(jnp.int32), axis=1)
    pick = (jnp.arange(row_count, dtype=jnp.int32)[:, None] == dest[None, :]).astype(jnp.bfloat16)
    gate = (group_weight[:, None] * expert_weight).astype(jnp.bfloat16)
    named = local_choice[:, :, None] == jnp.arange(LANES, dtype=jnp.int32)
    gate_cols = jnp.sum(jnp.where(named, gate[:, :, None], 0), axis=1).astype(jnp.bfloat16)
    lane = lax.axis_index("tp")
    token_cols = lax.dynamic_slice_in_dim(tokens, lane * piece, piece, 1)
    cot_cols = lax.dynamic_slice_in_dim(cotangent, lane * piece, piece, 1)
    payload = jnp.concatenate([token_cols, cot_cols, gate_cols], axis=1)
    rows = jnp.dot(pick, payload, preferred_element_type=jnp.float32).astype(jnp.bfloat16)
    rows = lax.all_to_all(rows, "g", split_axis=0, concat_axis=0, tiled=True)
    rows = lax.all_gather(rows, ("e", "tp"), axis=0, tiled=False)
    rows = rows.reshape(EPG, lane_count, row_count, 2 * piece + LANES)
    all_rows = EPG * row_count
    arrived = jnp.concatenate(
        [rows[:, y, :, :piece].reshape(all_rows, piece) for y in range(lane_count)], axis=1
    )
    cot_rows = jnp.concatenate(
        [rows[:, y, :, piece : 2 * piece].reshape(all_rows, piece) for y in range(lane_count)],
        axis=1,
    )
    own = jnp.arange(LANES, dtype=jnp.int32) == lax.axis_index("e")
    gate_block = rows[:, 0, :, 2 * piece :].reshape(all_rows, LANES).astype(jnp.float32)
    gate_float = jnp.sum(jnp.where(own, gate_block, 0.0), axis=1, keepdims=True)
    first, second, third = w_gate[0], w_up[0], w_down[0]
    contract_cols = (((1,), (1,)), ((), ()))
    contract_rows = (((0,), (0,)), ((), ()))
    pre_gate = jnp.dot(arrived, first, preferred_element_type=jnp.float32)
    pre_up = jnp.dot(arrived, second, preferred_element_type=jnp.float32)
    back = lax.dot_general(cot_rows, third, contract_cols, preferred_element_type=jnp.float32)
    sigma = jax.nn.sigmoid(pre_gate)
    swish = pre_gate * sigma
    hidden = swish * pre_up
    gate_part = jnp.sum(hidden * back, axis=1, keepdims=True)
    scaled = gate_float * back
    grad_gate = (scaled * pre_up * sigma * (1.0 + pre_gate * (1.0 - sigma))).astype(jnp.bfloat16)
    grad_up = (scaled * swish).astype(jnp.bfloat16)
    weighted = (gate_float * hidden).astype(jnp.bfloat16)
    partial_rows = lax.dot_general(
        grad_gate, first, contract_cols, preferred_element_type=jnp.float32
    ) + lax.dot_general(grad_up, second, contract_cols, preferred_element_type=jnp.float32)
    partial_rows = partial_rows.astype(jnp.bfloat16)
    gate_out = jnp.where(own, gate_part, 0.0).astype(jnp.bfloat16)
    back_rows = jnp.stack(
        [
            jnp.concatenate([partial_rows[:, y * piece : (y + 1) * piece], gate_out], axis=1)
            for y in range(lane_count)
        ]
    )
    back_rows = back_rows.reshape(lane_count, EPG, row_count, piece + LANES).swapaxes(0, 1)
    back_rows = back_rows.reshape(EPG * lane_count, row_count, piece + LANES)
    returned = lax.psum_scatter(back_rows, ("e", "tp"), scatter_dimension=0, tiled=False)
    returned = lax.all_to_all(returned, "g", split_axis=0, concat_axis=0, tiled=True)
    first_grad = lax.dot_general(
        arrived, grad_gate, contract_rows, preferred_element_type=jnp.float32
    )
    second_grad = lax.dot_general(
        arrived, grad_up, contract_rows, preferred_element_type=jnp.float32
    )
    third_grad = lax.dot_general(
        weighted, cot_rows, contract_rows, preferred_element_type=jnp.float32
    )
    result = lax.dot_general(pick, returned, contract_rows, preferred_element_type=jnp.float32)
    token_grad = result[:, :piece]
    gate_grad = jnp.sum(jnp.where(named, result[:, None, piece:], 0.0), axis=2)
    gate_grad = gate_grad.astype(jnp.bfloat16).astype(jnp.float32)
    group_grad = jnp.sum(expert_weight * gate_grad, axis=1)
    expert_grad = group_weight[:, None] * gate_grad
    return (
        token_grad,
        group_grad,
        expert_grad,
        first_grad[None],
        second_grad[None],
        third_grad[None],
    )


def solution(mesh):
    lanes = mesh.shape["tp"]
    split = Mesh(mesh.devices.reshape(-1, EPG, lanes), ("g", "e", "tp"))
    ep = ("g", "e")
    in_specs = (
        P(ep, None),
        P(ep, None),
        P(ep),
        P(ep, None),
        P(ep),
        P(ep, None),
        P(ep, None, "tp"),
        P(ep, None, "tp"),
        P(ep, "tp", None),
    )
    out_specs = (
        P(ep, "tp"),
        P(ep),
        P(ep, None),
        P(ep, None, "tp"),
        P(ep, None, "tp"),
        P(ep, "tp", None),
    )
    return jax.shard_map(
        shards, mesh=split, in_specs=in_specs, out_specs=out_specs, check_vma=False
    )
```

```python
import functools

import jax
import jax.numpy as jnp
from jax import lax
from jax.experimental import pallas as pl
from jax.experimental.pallas import tpu as pltpu
from jax.sharding import Mesh, PartitionSpec as P

EPG = 4
LANES = 128

MESH = pl.DeviceIdType.MESH


def place():
    g, e, y = lax.axis_index("g"), lax.axis_index("e"), lax.axis_index("tp")
    x, c = e // 2, e % 2
    return g, e, y, x, c


def greet(devices):
    barrier = pltpu.get_barrier_semaphore()
    for device in devices:
        pl.semaphore_signal(barrier, inc=1, device_id=device, device_id_type=MESH)
    pl.semaphore_wait(barrier, len(devices))


class Copies:
    def __init__(self, send_sem, recv_sem):
        self.send_sem, self.recv_sem, self.made = send_sem, recv_sem, []

    def start(self, src, dst, device):
        number = len(self.made)
        copy = pltpu.make_async_remote_copy(
            src_ref=src,
            dst_ref=dst,
            send_sem=self.send_sem.at[number],
            recv_sem=self.recv_sem.at[number],
            device_id=device,
            device_id_type=MESH,
        )
        copy.start()
        self.made.append(copy)
        return copy

    def finish(self):
        for copy in self.made:
            copy.wait_send()


def window(start, size, unit):
    return pl.ds(pl.multiple_of(start, unit), size)


def forward_count(groups, lanes):
    return (groups - 1) * 3 + groups * (3 * (lanes - 1) + 9)


def forward_kernel(groups, lanes, cap, piece, tok_in, cot_in, gate_in, tok, cot, gate, send, recv, loc):
    g, e, y, x, c = place()
    rows = groups * cap
    ex, ec, exc = (1 - x) * 2 + c, x * 2 + (1 - c), (1 - x) * 2 + (1 - c)
    others = [(g, e, lax.rem(y + r, lanes)) for r in range(1, lanes)]
    greet(
        [(lax.rem(g + d, groups), e, y) for d in range(1, groups)]
        + others
        + [(g, ex, y), (g, ec, y), (g, exc, y)]
    )
    copies = Copies(send, recv)
    cols = window(y * piece, piece, LANES)

    def block(ref, owner, source, columns=slice(None)):
        return ref.at[window(owner * rows + source * cap, cap, 16), columns]

    def inner(ref, group):
        return ref.at[window(group * cap, cap, 16), :]

    first = []
    pairs = ((tok_in, tok, cols), (cot_in, cot, cols), (gate_in, gate, slice(None)))
    for d in range(groups):
        target = lax.rem(g - d + groups, groups)
        made = []
        for i, (src, dst, columns) in enumerate(pairs):
            if d == 0:
                copy = pltpu.make_async_copy(inner(src, g), block(dst, e, g, columns), loc.at[i])
                copy.start()
            else:
                copy = copies.start(inner(src, target), block(dst, e, g, columns), (target, e, y))
            made.append(copy)
        first.append(made)
    state = [dict() for _ in range(groups)]
    last = []

    def stage_a(d):
        source = lax.rem(g + d, groups)
        for copy in first[d]:
            if d == 0:
                copy.wait()
            else:
                copy.wait_recv()
        own_t, own_c = block(tok, e, source, cols), block(cot, e, source, cols)
        state[d]["tl"] = [copies.start(own_t, own_t, device) for device in others]
        state[d]["cx"] = copies.start(own_c, own_c, (g, ex, y))
        state[d]["cl"] = [copies.start(own_c, own_c, device) for device in others]
        own_g = block(gate, e, source)
        for peer in (ex, ec, exc):
            last.append(copies.start(own_g, own_g, (g, peer, y)))

    def stage_b(d):
        source = lax.rem(g + d, groups)
        for copy in state[d]["tl"]:
            copy.wait_recv()
        full = block(tok, e, source)
        state[d]["tx"] = copies.start(full, full, (g, ex, y))
        state[d]["cx"].wait_recv()
        part = block(cot, ex, source, cols)
        state[d]["cxl"] = [copies.start(part, part, device) for device in others]
        last.append(copies.start(full, full, (g, ec, y)))

    def stage_c(d):
        source = lax.rem(g + d, groups)
        for copy in state[d]["cl"]:
            copy.wait_recv()
        full = block(cot, e, source)
        last.append(copies.start(full, full, (g, ec, y)))
        state[d]["tx"].wait_recv()
        full = block(tok, ex, source)
        last.append(copies.start(full, full, (g, ec, y)))
        for copy in state[d]["cxl"]:
            copy.wait_recv()
        full = block(cot, ex, source)
        last.append(copies.start(full, full, (g, ec, y)))

    for step in range(groups + 2):
        if step < groups:
            stage_a(step)
        if 0 <= step - 1 < groups:
            stage_b(step - 1)
        if 0 <= step - 2 < groups:
            stage_c(step - 2)
    for copy in last:
        copy.wait_recv()
    copies.finish()


def forward(tok_in, cot_in, gate_in, groups, lanes, cap, piece):
    all_rows = EPG * groups * cap
    count = forward_count(groups, lanes)
    vmem = pl.BlockSpec(memory_space=pltpu.VMEM)
    return pl.pallas_call(
        functools.partial(forward_kernel, groups, lanes, cap, piece),
        out_shape=(
            jax.ShapeDtypeStruct((all_rows, lanes * piece), jnp.bfloat16),
            jax.ShapeDtypeStruct((all_rows, lanes * piece), jnp.bfloat16),
            jax.ShapeDtypeStruct((all_rows, LANES), jnp.bfloat16),
        ),
        in_specs=[vmem] * 3,
        out_specs=(vmem,) * 3,
        scratch_shapes=[
            pltpu.SemaphoreType.DMA((count,)),
            pltpu.SemaphoreType.DMA((count,)),
            pltpu.SemaphoreType.DMA((3,)),
        ],
        compiler_params=pltpu.CompilerParams(collective_id=0, has_side_effects=True),
        name="forward_exchange",
    )(tok_in, cot_in, gate_in)


def add(*parts):
    total = parts[0].astype(jnp.float32)
    for part in parts[1:]:
        total = total + part.astype(jnp.float32)
    return total.astype(jnp.bfloat16)


def return_kernel(
    groups, lanes, cap, wide0, wide1, part, out, rc, s1, rx0, s2a, rl0, rl1, s2b, rx1, done, send, recv
):
    g, e, y, x, c = place()
    rows = groups * cap
    ex, ec = (1 - x) * 2 + c, x * 2 + (1 - c)
    others = [(g, e, lax.rem(y + r, lanes)) for r in range(1, lanes)]
    greet(
        [(lax.rem(g + d, groups), e, y) for d in range(1, groups)]
        + others
        + [(g, ex, y), (g, ec, y)]
    )
    copies = Copies(send, recv)
    all0 = lanes * wide0
    head, tail = pl.ds(0, all0), pl.ds(all0, lanes * wide1)

    def at(index, source):
        return window(index * rows + source * cap, cap, 16)

    def lane0(lane):
        return window(lane * wide0, wide0, LANES)

    def lane1(lane):
        return window(all0 + lane * wide1, wide1, LANES)

    order = list(range(1, groups)) + [0]
    sources = [lax.rem(g + d, groups) for d in order]
    state = [dict() for _ in order]
    for i, s in enumerate(sources):
        state[i]["core"] = [
            copies.start(part.at[at(2 * k + 1 - c, s), :], rc.at[at(k, s), :], (g, ec, y))
            for k in range(2)
        ]

    def stage_a(i):
        s = sources[i]
        for k in range(2):
            state[i]["core"][k].wait_recv()
            for columns in (head, tail):
                s1[at(k, s), columns] = add(part[at(2 * k + c, s), columns], rc[at(k, s), columns])
        state[i]["x0"] = copies.start(s1.at[at(1 - x, s), head], rx0.at[at(0, s), :], (g, ex, y))
        state[i]["l1"] = [
            copies.start(
                s1.at[at(k, s), lane1(device[2])], rl1.at[at(2 * r + k, s), :], device
            )
            for r, device in enumerate(others)
            for k in range(2)
        ]

    def stage_b(i):
        s = sources[i]
        state[i]["x0"].wait_recv()
        s2a[at(0, s), :] = add(s1[at(x, s), head], rx0[at(0, s), :])
        state[i]["l0"] = [
            copies.start(s2a.at[at(0, s), lane0(device[2])], rl0.at[at(r, s), :], device)
            for r, device in enumerate(others)
        ]
        for copy in state[i]["l1"]:
            copy.wait_recv()
        for k in range(2):
            s2b[at(k, s), :] = add(
                s1[at(k, s), lane1(y)], *[rl1[at(2 * r + k, s), :] for r in range(lanes - 1)]
            )
        state[i]["x1"] = copies.start(s2b.at[at(1 - x, s), :], rx1.at[at(0, s), :], (g, ex, y))

    def stage_c(i):
        s = sources[i]
        target = out if order[i] == 0 else done
        for copy in state[i]["l0"]:
            copy.wait_recv()
        target[at(0, s), pl.ds(0, wide0)] = add(
            s2a[at(0, s), lane0(y)], *[rl0[at(r, s), :] for r in range(lanes - 1)]
        )
        state[i]["x1"].wait_recv()
        target[at(0, s), pl.ds(wide0, wide1)] = add(s2b[at(x, s), :], rx1[at(0, s), :])
        if order[i] != 0:
            state[i]["z"] = copies.start(done.at[at(0, s), :], out.at[at(0, g), :], (s, e, y))

    for step in range(groups + 2):
        if step < groups:
            stage_a(step)
        if 0 <= step - 1 < groups:
            stage_b(step - 1)
        if 0 <= step - 2 < groups:
            stage_c(step - 2)
    for i in range(groups):
        if order[i] != 0:
            state[i]["z"].wait_recv()
    copies.finish()


def give_back(part, groups, lanes, cap, wide0, wide1):
    rows = groups * cap
    count = (groups - 1) + groups * (4 + 3 * (lanes - 1))
    vmem = pl.BlockSpec(memory_space=pltpu.VMEM)
    wide = lanes * (wide0 + wide1)
    far = max(lanes - 1, 1)

    def buffer(height, width):
        return pltpu.VMEM((height, width), jnp.bfloat16)

    return pl.pallas_call(
        functools.partial(return_kernel, groups, lanes, cap, wide0, wide1),
        out_shape=jax.ShapeDtypeStruct((rows, wide0 + wide1), jnp.bfloat16),
        in_specs=[vmem],
        out_specs=vmem,
        scratch_shapes=[
            buffer(2 * rows, wide),
            buffer(2 * rows, wide),
            buffer(rows, lanes * wide0),
            buffer(rows, lanes * wide0),
            buffer(far * rows, wide0),
            buffer(far * 2 * rows, wide1),
            buffer(2 * rows, wide1),
            buffer(rows, wide1),
            buffer(rows, wide0 + wide1),
            pltpu.SemaphoreType.DMA((count,)),
            pltpu.SemaphoreType.DMA((count,)),
        ],
        compiler_params=pltpu.CompilerParams(collective_id=1, has_side_effects=True),
        name="return_exchange",
    )(part)


def shards(
    tokens, cotangent, group_weight, expert_weight, group_choice, local_choice, w_gate, w_up, w_down
):
    token_count, feature_count = tokens.shape
    pick_count = expert_weight.shape[1]
    group_count = lax.axis_size("g")
    lane_count = lax.axis_size("tp")
    expert_count = group_count * EPG
    capacity = pick_count * (3 * token_count // (2 * expert_count))
    group_cap = -(-(EPG * capacity // pick_count) // 16) * 16
    row_count = group_count * group_cap
    piece = feature_count // lane_count
    order = jnp.arange(token_count, dtype=jnp.int32)
    same = (group_choice[:, None] == group_choice[None, :]) & (order[:, None] > order[None, :])
    dest = group_choice * group_cap + jnp.sum(same.astype(jnp.int32), axis=1)
    pick = (jnp.arange(row_count, dtype=jnp.int32)[:, None] == dest[None, :]).astype(jnp.bfloat16)
    gate = (group_weight[:, None] * expert_weight).astype(jnp.bfloat16)
    named = local_choice[:, :, None] == jnp.arange(LANES, dtype=jnp.int32)
    gate_cols = jnp.sum(jnp.where(named, gate[:, :, None], 0), axis=1).astype(jnp.bfloat16)
    lane = lax.axis_index("tp")
    token_cols = lax.dynamic_slice_in_dim(tokens, lane * piece, piece, 1)
    cot_cols = lax.dynamic_slice_in_dim(cotangent, lane * piece, piece, 1)
    payload = jnp.concatenate([token_cols, cot_cols, gate_cols], axis=1)
    rows = jnp.dot(pick, payload, preferred_element_type=jnp.float32).astype(jnp.bfloat16)
    arrived, cot_rows, gate_block = forward(
        rows[:, :piece],
        rows[:, piece : 2 * piece],
        rows[:, 2 * piece :],
        group_count,
        lane_count,
        group_cap,
        piece,
    )
    own = jnp.arange(LANES, dtype=jnp.int32) == lax.axis_index("e")
    gate_block = gate_block.astype(jnp.float32)
    gate_float = jnp.sum(jnp.where(own, gate_block, 0.0), axis=1, keepdims=True)
    first, second, third = w_gate[0], w_up[0], w_down[0]
    contract_cols = (((1,), (1,)), ((), ()))
    contract_rows = (((0,), (0,)), ((), ()))
    pre_gate = jnp.dot(arrived, first, preferred_element_type=jnp.float32)
    pre_up = jnp.dot(arrived, second, preferred_element_type=jnp.float32)
    back = lax.dot_general(cot_rows, third, contract_cols, preferred_element_type=jnp.float32)
    sigma = jax.nn.sigmoid(pre_gate)
    swish = pre_gate * sigma
    hidden = swish * pre_up
    gate_part = jnp.sum(hidden * back, axis=1, keepdims=True)
    scaled = gate_float * back
    grad_gate = (scaled * pre_up * sigma * (1.0 + pre_gate * (1.0 - sigma))).astype(jnp.bfloat16)
    grad_up = (scaled * swish).astype(jnp.bfloat16)
    weighted = (gate_float * hidden).astype(jnp.bfloat16)
    partial_rows = lax.dot_general(
        grad_gate, first, contract_cols, preferred_element_type=jnp.float32
    ) + lax.dot_general(grad_up, second, contract_cols, preferred_element_type=jnp.float32)
    partial_rows = partial_rows.astype(jnp.bfloat16)
    gate_out = jnp.where(own, gate_part, 0.0).astype(jnp.bfloat16)
    wide1 = (piece + LANES) // (2 * LANES) * LANES
    wide0 = piece + LANES - wide1
    back_rows = jnp.concatenate(
        [partial_rows[:, y * piece : y * piece + wide0] for y in range(lane_count)]
        + [
            column
            for y in range(lane_count)
            for column in (partial_rows[:, y * piece + wide0 : (y + 1) * piece], gate_out)
        ],
        axis=1,
    )
    returned = give_back(back_rows, group_count, lane_count, group_cap, wide0, wide1)
    first_grad = lax.dot_general(
        arrived, grad_gate, contract_rows, preferred_element_type=jnp.float32
    )
    second_grad = lax.dot_general(
        arrived, grad_up, contract_rows, preferred_element_type=jnp.float32
    )
    third_grad = lax.dot_general(
        weighted, cot_rows, contract_rows, preferred_element_type=jnp.float32
    )
    result = lax.dot_general(pick, returned, contract_rows, preferred_element_type=jnp.float32)
    token_grad = result[:, :piece]
    gate_grad = jnp.sum(jnp.where(named, result[:, None, piece:], 0.0), axis=2)
    gate_grad = gate_grad.astype(jnp.bfloat16).astype(jnp.float32)
    group_grad = jnp.sum(expert_weight * gate_grad, axis=1)
    expert_grad = group_weight[:, None] * gate_grad
    return (
        token_grad,
        group_grad,
        expert_grad,
        first_grad[None],
        second_grad[None],
        third_grad[None],
    )


def solution(mesh):
    lanes = mesh.shape["tp"]
    split = Mesh(mesh.devices.reshape(-1, EPG, lanes), ("g", "e", "tp"))
    ep = ("g", "e")
    in_specs = (
        P(ep, None),
        P(ep, None),
        P(ep),
        P(ep, None),
        P(ep),
        P(ep, None),
        P(ep, None, "tp"),
        P(ep, None, "tp"),
        P(ep, "tp", None),
    )
    out_specs = (
        P(ep, "tp"),
        P(ep),
        P(ep, None),
        P(ep, None, "tp"),
        P(ep, None, "tp"),
        P(ep, "tp", None),
    )
    return jax.shard_map(
        shards, mesh=split, in_specs=in_specs, out_specs=out_specs, check_vma=False
    )
```

```python
import functools

import jax
import jax.numpy as jnp
from jax import lax
from jax.experimental import pallas as pl
from jax.experimental.pallas import tpu as pltpu
from jax.sharding import Mesh, PartitionSpec as P

EPG = 4
LANES = 128

MESH = pl.DeviceIdType.MESH


def place():
    g, e, y = lax.axis_index("g"), lax.axis_index("e"), lax.axis_index("tp")
    x, c = e // 2, e % 2
    return g, e, y, x, c


def partner(g, d, groups, sign):
    if groups & (groups - 1):
        return lax.rem(g + sign * d + groups, groups)
    met, bit = g, 1
    while bit < groups:
        if d & bit:
            met = met + bit - 2 * bit * ((g // bit) % 2)
        bit *= 2
    return met


def greet(devices):
    barrier = pltpu.get_barrier_semaphore()
    for device in devices:
        pl.semaphore_signal(barrier, inc=1, device_id=device, device_id_type=MESH)
    pl.semaphore_wait(barrier, len(devices))


class Copies:
    def __init__(self, send_sem, recv_sem):
        self.send_sem, self.recv_sem, self.made = send_sem, recv_sem, []

    def start(self, src, dst, device):
        number = len(self.made)
        copy = pltpu.make_async_remote_copy(
            src_ref=src,
            dst_ref=dst,
            send_sem=self.send_sem.at[number],
            recv_sem=self.recv_sem.at[number],
            device_id=device,
            device_id_type=MESH,
        )
        copy.start()
        self.made.append(copy)
        return copy

    def finish(self):
        for copy in self.made:
            copy.wait_send()


def window(start, size, unit):
    return pl.ds(pl.multiple_of(start, unit), size)


def forward_count(groups, lanes):
    return (groups - 1) * 3 + groups * (3 * (lanes - 1) + 9)


def forward_kernel(groups, lanes, cap, piece, tok_in, cot_in, gate_in, tok, cot, gate, send, recv, loc):
    g, e, y, x, c = place()
    rows = groups * cap
    ex, ec, exc = (1 - x) * 2 + c, x * 2 + (1 - c), (1 - x) * 2 + (1 - c)
    others = [(g, e, lax.rem(y + r, lanes)) for r in range(1, lanes)]
    greet(
        [(lax.rem(g + d, groups), e, y) for d in range(1, groups)]
        + others
        + [(g, ex, y), (g, ec, y), (g, exc, y)]
    )
    copies = Copies(send, recv)
    cols = window(y * piece, piece, LANES)

    def block(ref, owner, source, columns=slice(None)):
        return ref.at[window(owner * rows + source * cap, cap, 16), columns]

    def inner(ref, group):
        return ref.at[window(group * cap, cap, 16), :]

    first = []
    pairs = ((tok_in, tok, cols), (cot_in, cot, cols), (gate_in, gate, slice(None)))
    for d in range(groups):
        target = partner(g, d, groups, -1)
        made = []
        for i, (src, dst, columns) in enumerate(pairs):
            if d == 0:
                copy = pltpu.make_async_copy(inner(src, g), block(dst, e, g, columns), loc.at[i])
                copy.start()
            else:
                copy = copies.start(inner(src, target), block(dst, e, g, columns), (target, e, y))
            made.append(copy)
        first.append(made)
    state = [dict() for _ in range(groups)]
    last = []

    def stage_a(d):
        source = partner(g, d, groups, 1)
        for copy in first[d]:
            if d == 0:
                copy.wait()
            else:
                copy.wait_recv()
        own_t, own_c = block(tok, e, source, cols), block(cot, e, source, cols)
        state[d]["tl"] = [copies.start(own_t, own_t, device) for device in others]
        state[d]["cx"] = copies.start(own_c, own_c, (g, ex, y))
        state[d]["cl"] = [copies.start(own_c, own_c, device) for device in others]
        own_g = block(gate, e, source)
        for peer in (ex, ec, exc):
            last.append(copies.start(own_g, own_g, (g, peer, y)))

    def stage_b(d):
        source = partner(g, d, groups, 1)
        for copy in state[d]["tl"]:
            copy.wait_recv()
        full = block(tok, e, source)
        state[d]["tx"] = copies.start(full, full, (g, ex, y))
        state[d]["cx"].wait_recv()
        part = block(cot, ex, source, cols)
        state[d]["cxl"] = [copies.start(part, part, device) for device in others]
        last.append(copies.start(full, full, (g, ec, y)))

    def stage_c(d):
        source = partner(g, d, groups, 1)
        for copy in state[d]["cl"]:
            copy.wait_recv()
        full = block(cot, e, source)
        last.append(copies.start(full, full, (g, ec, y)))
        state[d]["tx"].wait_recv()
        full = block(tok, ex, source)
        last.append(copies.start(full, full, (g, ec, y)))
        for copy in state[d]["cxl"]:
            copy.wait_recv()
        full = block(cot, ex, source)
        last.append(copies.start(full, full, (g, ec, y)))

    for step in range(groups + 2):
        if step < groups:
            stage_a(step)
        if 0 <= step - 1 < groups:
            stage_b(step - 1)
        if 0 <= step - 2 < groups:
            stage_c(step - 2)
    for copy in last:
        copy.wait_recv()
    copies.finish()


def forward(tok_in, cot_in, gate_in, groups, lanes, cap, piece):
    all_rows = EPG * groups * cap
    count = forward_count(groups, lanes)
    vmem = pl.BlockSpec(memory_space=pltpu.VMEM)
    return pl.pallas_call(
        functools.partial(forward_kernel, groups, lanes, cap, piece),
        out_shape=(
            jax.ShapeDtypeStruct((all_rows, lanes * piece), jnp.bfloat16),
            jax.ShapeDtypeStruct((all_rows, lanes * piece), jnp.bfloat16),
            jax.ShapeDtypeStruct((all_rows, LANES), jnp.bfloat16),
        ),
        in_specs=[vmem] * 3,
        out_specs=(vmem,) * 3,
        scratch_shapes=[
            pltpu.SemaphoreType.DMA((count,)),
            pltpu.SemaphoreType.DMA((count,)),
            pltpu.SemaphoreType.DMA((3,)),
        ],
        compiler_params=pltpu.CompilerParams(collective_id=0, has_side_effects=True),
        name="forward_exchange",
    )(tok_in, cot_in, gate_in)


def add(*parts):
    total = parts[0].astype(jnp.float32)
    for part in parts[1:]:
        total = total + part.astype(jnp.float32)
    return total.astype(jnp.bfloat16)


def return_kernel(
    groups, lanes, cap, wide0, wide1, part, out, rc, s1, rx0, s2a, rl0, rl1, s2b, rx1, done, send, recv
):
    g, e, y, x, c = place()
    rows = groups * cap
    ex, ec = (1 - x) * 2 + c, x * 2 + (1 - c)
    others = [(g, e, lax.rem(y + r, lanes)) for r in range(1, lanes)]
    greet(
        [(lax.rem(g + d, groups), e, y) for d in range(1, groups)]
        + others
        + [(g, ex, y), (g, ec, y)]
    )
    copies = Copies(send, recv)
    all0 = lanes * wide0
    head, tail = pl.ds(0, all0), pl.ds(all0, lanes * wide1)

    def at(index, source):
        return window(index * rows + source * cap, cap, 16)

    def lane0(lane):
        return window(lane * wide0, wide0, LANES)

    def lane1(lane):
        return window(all0 + lane * wide1, wide1, LANES)

    order = list(range(groups // 2, groups)) + list(range(1, groups // 2)) + [0]
    sources = [partner(g, d, groups, 1) for d in order]
    state = [dict() for _ in order]
    for i, s in enumerate(sources):
        state[i]["core"] = [
            copies.start(part.at[at(2 * k + 1 - c, s), :], rc.at[at(k, s), :], (g, ec, y))
            for k in range(2)
        ]

    def stage_a(i):
        s = sources[i]
        for k in range(2):
            state[i]["core"][k].wait_recv()
            for columns in (head, tail):
                s1[at(k, s), columns] = add(part[at(2 * k + c, s), columns], rc[at(k, s), columns])
        state[i]["x0"] = copies.start(s1.at[at(1 - x, s), head], rx0.at[at(0, s), :], (g, ex, y))
        state[i]["l1"] = [
            copies.start(
                s1.at[at(k, s), lane1(device[2])], rl1.at[at(2 * r + k, s), :], device
            )
            for r, device in enumerate(others)
            for k in range(2)
        ]

    def stage_b(i):
        s = sources[i]
        state[i]["x0"].wait_recv()
        s2a[at(0, s), :] = add(s1[at(x, s), head], rx0[at(0, s), :])
        state[i]["l0"] = [
            copies.start(s2a.at[at(0, s), lane0(device[2])], rl0.at[at(r, s), :], device)
            for r, device in enumerate(others)
        ]
        for copy in state[i]["l1"]:
            copy.wait_recv()
        for k in range(2):
            s2b[at(k, s), :] = add(
                s1[at(k, s), lane1(y)], *[rl1[at(2 * r + k, s), :] for r in range(lanes - 1)]
            )
        state[i]["x1"] = copies.start(s2b.at[at(1 - x, s), :], rx1.at[at(0, s), :], (g, ex, y))

    def stage_c(i):
        s = sources[i]
        target = out if order[i] == 0 else done
        for copy in state[i]["l0"]:
            copy.wait_recv()
        target[at(0, s), pl.ds(0, wide0)] = add(
            s2a[at(0, s), lane0(y)], *[rl0[at(r, s), :] for r in range(lanes - 1)]
        )
        state[i]["x1"].wait_recv()
        target[at(0, s), pl.ds(wide0, wide1)] = add(s2b[at(x, s), :], rx1[at(0, s), :])
        if order[i] != 0:
            state[i]["z"] = copies.start(done.at[at(0, s), :], out.at[at(0, g), :], (s, e, y))

    for step in range(groups + 2):
        if step < groups:
            stage_a(step)
        if 0 <= step - 1 < groups:
            stage_b(step - 1)
        if 0 <= step - 2 < groups:
            stage_c(step - 2)
    for i in range(groups):
        if order[i] != 0:
            state[i]["z"].wait_recv()
    copies.finish()


def give_back(part, groups, lanes, cap, wide0, wide1):
    rows = groups * cap
    count = (groups - 1) + groups * (4 + 3 * (lanes - 1))
    vmem = pl.BlockSpec(memory_space=pltpu.VMEM)
    wide = lanes * (wide0 + wide1)
    far = max(lanes - 1, 1)

    def buffer(height, width):
        return pltpu.VMEM((height, width), jnp.bfloat16)

    return pl.pallas_call(
        functools.partial(return_kernel, groups, lanes, cap, wide0, wide1),
        out_shape=jax.ShapeDtypeStruct((rows, wide0 + wide1), jnp.bfloat16),
        in_specs=[vmem],
        out_specs=vmem,
        scratch_shapes=[
            buffer(2 * rows, wide),
            buffer(2 * rows, wide),
            buffer(rows, lanes * wide0),
            buffer(rows, lanes * wide0),
            buffer(far * rows, wide0),
            buffer(far * 2 * rows, wide1),
            buffer(2 * rows, wide1),
            buffer(rows, wide1),
            buffer(rows, wide0 + wide1),
            pltpu.SemaphoreType.DMA((count,)),
            pltpu.SemaphoreType.DMA((count,)),
        ],
        compiler_params=pltpu.CompilerParams(collective_id=1, has_side_effects=True),
        name="return_exchange",
    )(part)


def shards(
    tokens, cotangent, group_weight, expert_weight, group_choice, local_choice, w_gate, w_up, w_down
):
    token_count, feature_count = tokens.shape
    pick_count = expert_weight.shape[1]
    group_count = lax.axis_size("g")
    lane_count = lax.axis_size("tp")
    expert_count = group_count * EPG
    capacity = pick_count * (3 * token_count // (2 * expert_count))
    group_cap = -(-(EPG * capacity // pick_count) // 16) * 16
    row_count = group_count * group_cap
    piece = feature_count // lane_count
    order = jnp.arange(token_count, dtype=jnp.int32)
    same = (group_choice[:, None] == group_choice[None, :]) & (order[:, None] > order[None, :])
    dest = group_choice * group_cap + jnp.sum(same.astype(jnp.int32), axis=1)
    pick = (jnp.arange(row_count, dtype=jnp.int32)[:, None] == dest[None, :]).astype(jnp.bfloat16)
    gate = (group_weight[:, None] * expert_weight).astype(jnp.bfloat16)
    named = local_choice[:, :, None] == jnp.arange(LANES, dtype=jnp.int32)
    gate_cols = jnp.sum(jnp.where(named, gate[:, :, None], 0), axis=1).astype(jnp.bfloat16)
    lane = lax.axis_index("tp")
    token_cols = lax.dynamic_slice_in_dim(tokens, lane * piece, piece, 1)
    cot_cols = lax.dynamic_slice_in_dim(cotangent, lane * piece, piece, 1)
    payload = jnp.concatenate([token_cols, cot_cols, gate_cols], axis=1)
    rows = jnp.dot(pick, payload, preferred_element_type=jnp.float32).astype(jnp.bfloat16)
    arrived, cot_rows, gate_block = forward(
        rows[:, :piece],
        rows[:, piece : 2 * piece],
        rows[:, 2 * piece :],
        group_count,
        lane_count,
        group_cap,
        piece,
    )
    own = jnp.arange(LANES, dtype=jnp.int32) == lax.axis_index("e")
    gate_block = gate_block.astype(jnp.float32)
    gate_float = jnp.sum(jnp.where(own, gate_block, 0.0), axis=1, keepdims=True)
    first, second, third = w_gate[0], w_up[0], w_down[0]
    contract_cols = (((1,), (1,)), ((), ()))
    contract_rows = (((0,), (0,)), ((), ()))
    pre_gate = jnp.dot(arrived, first, preferred_element_type=jnp.float32)
    pre_up = jnp.dot(arrived, second, preferred_element_type=jnp.float32)
    back = lax.dot_general(cot_rows, third, contract_cols, preferred_element_type=jnp.float32)
    sigma = jax.nn.sigmoid(pre_gate)
    swish = pre_gate * sigma
    hidden = swish * pre_up
    gate_part = jnp.sum(hidden * back, axis=1, keepdims=True)
    scaled = gate_float * back
    grad_gate = (scaled * pre_up * sigma * (1.0 + pre_gate * (1.0 - sigma))).astype(jnp.bfloat16)
    grad_up = (scaled * swish).astype(jnp.bfloat16)
    weighted = (gate_float * hidden).astype(jnp.bfloat16)
    partial_rows = lax.dot_general(
        grad_gate, first, contract_cols, preferred_element_type=jnp.float32
    ) + lax.dot_general(grad_up, second, contract_cols, preferred_element_type=jnp.float32)
    partial_rows = partial_rows.astype(jnp.bfloat16)
    gate_out = jnp.where(own, gate_part, 0.0).astype(jnp.bfloat16)
    wide1 = (piece + LANES) // (2 * LANES) * LANES
    wide0 = piece + LANES - wide1
    back_rows = jnp.concatenate(
        [partial_rows[:, y * piece : y * piece + wide0] for y in range(lane_count)]
        + [
            column
            for y in range(lane_count)
            for column in (partial_rows[:, y * piece + wide0 : (y + 1) * piece], gate_out)
        ],
        axis=1,
    )
    returned = give_back(back_rows, group_count, lane_count, group_cap, wide0, wide1)
    first_grad = lax.dot_general(
        arrived, grad_gate, contract_rows, preferred_element_type=jnp.float32
    )
    second_grad = lax.dot_general(
        arrived, grad_up, contract_rows, preferred_element_type=jnp.float32
    )
    third_grad = lax.dot_general(
        weighted, cot_rows, contract_rows, preferred_element_type=jnp.float32
    )
    result = lax.dot_general(pick, returned, contract_rows, preferred_element_type=jnp.float32)
    token_grad = result[:, :piece]
    gate_grad = jnp.sum(jnp.where(named, result[:, None, piece:], 0.0), axis=2)
    gate_grad = gate_grad.astype(jnp.bfloat16).astype(jnp.float32)
    group_grad = jnp.sum(expert_weight * gate_grad, axis=1)
    expert_grad = group_weight[:, None] * gate_grad
    return (
        token_grad,
        group_grad,
        expert_grad,
        first_grad[None],
        second_grad[None],
        third_grad[None],
    )


def solution(mesh):
    lanes = mesh.shape["tp"]
    split = Mesh(mesh.devices.reshape(-1, EPG, lanes), ("g", "e", "tp"))
    ep = ("g", "e")
    in_specs = (
        P(ep, None),
        P(ep, None),
        P(ep),
        P(ep, None),
        P(ep),
        P(ep, None),
        P(ep, None, "tp"),
        P(ep, None, "tp"),
        P(ep, "tp", None),
    )
    out_specs = (
        P(ep, "tp"),
        P(ep),
        P(ep, None),
        P(ep, None, "tp"),
        P(ep, None, "tp"),
        P(ep, "tp", None),
    )
    return jax.shard_map(
        shards, mesh=split, in_specs=in_specs, out_specs=out_specs, check_vma=False
    )
```
